32 devices in a mesh: ep: 8 (over z, y), tp: 4 (over x, core).
Axes of the slice: x: 2, y: 2, z: 4, core: 2. Of those that a mesh axis runs over, the one named last changes fastest.
Arguments:
- queries: bfloat16 [2048, 1024], P('ep', 'tp'), may hold values from -200 to 200
- keys: bfloat16 [2048, 512], P('ep', 'tp'), may hold values from -5 to 5
- values: bfloat16 [2048, 512], P('ep', 'tp'), may hold values from -6 to 6
- log_gates: float32 [2048, 16], P('ep', 'tp'), may hold values from -2048 to 0, as said below
- out_weight: bfloat16 [1024, 2048], P('tp'), may hold values from -0.1875 to 0.1875
- moe_rows: bfloat16 [2048, 2048], P('ep'), may hold values from -6 to 6
- norm_gain: float32 [2048], replicated, may hold values from 0.1 to 1.9
- experts: int32 [2048, 2], P('ep'), may hold values from 0 to 7, all different within a row; in each aligned block of 256 rows (0 to 255, 256 to 511, ...) at most 128 rows name the same one
- expert_weights: float32 [2048, 2], P('ep'), may hold values from 0.2 to 1
- w_gate: bfloat16 [8, 2048, 1024], P('ep', None, 'tp'), may hold values from -0.125 to 0.125
- w_up: bfloat16 [8, 2048, 1024], P('ep', None, 'tp'), may hold values from -0.125 to 0.125
- w_down: bfloat16 [8, 1024, 2048], P('ep', 'tp'), may hold values from -0.1875 to 0.1875
Outputs:
- mixed: bfloat16 [2048, 2048], P(('ep', 'tp'))
- moe_out: bfloat16 [2048, 2048], P('ep', 'tp')
The draws below stay inside these ranges and needn't reach their ends.
Inputs may be any that keep to these rules, and one draw needn't show every extreme that they name: Each token names 2 different experts; within the rows of one index of ep (aligned blocks of 256 rows) no expert is named more than 128 times, a bound that some block reaches. `log_gates`: Non-increasing along positions in every head.
All inputs are finite; a program needn't handle non-finite values.
Results may differ from the reference program's by a relative error of at most 0.01195.
Values may be sent and summed in bfloat16 or wider, within the bound.
A program may use at most 128 MiB of HBM per device.

```python
import math
import jax
import jax.numpy as jnp
import numpy as np
from jax import lax

D = 2048
HD = 64
HEADS = 16
KV = 8
FF = 1024
TOPK = 2
TOK_DEV = 256
MOE_EP = 256
LEAD_SPAN_LENGTH = 2048
MTOK = 2048
EXPERTS = 8
CAP = 128
N_EP = 8
N_TP = 4


def attention_pair(key):
    reference_level = jax.random.fold_in(key, 11)
    query_key, key_key = jax.random.split(reference_level, 2)
    key_rows = jnp.clip(jax.random.normal(key_key, (LEAD_SPAN_LENGTH, KV * HD), jnp.float32), -5.0, 5.0)
    query_rows = jnp.clip(jax.random.normal(query_key, (LEAD_SPAN_LENGTH, HEADS * HD), jnp.float32), -5.0, 5.0)
    return (query_rows, key_rows)


def draw_queries(key, part):
    return attention_pair(key)[0].astype(jnp.bfloat16)


def draw_keys(key, part):
    return attention_pair(key)[1].astype(jnp.bfloat16)


def draw_log_gates(key, part):
    reference_level = jax.random.fold_in(key, 23)
    arrangement_prng_seed, iteration_prng_seed, tile_prng_seed, spike_prng_seed, objective_prng_seed = jax.random.split(reference_level, 5)
    head_rank = jax.random.permutation(arrangement_prng_seed, HEADS)
    delay_multiplier = head_rank < HEADS // 2
    per_step = jnp.exp(jax.random.uniform(iteration_prng_seed, (LEAD_SPAN_LENGTH, HEADS), jnp.float32, jnp.log(0.5), jnp.log(2.0)))
    block_factor = jnp.exp(jax.random.uniform(tile_prng_seed, (LEAD_SPAN_LENGTH // TOK_DEV, HEADS), jnp.float32, jnp.log(0.7), jnp.log(2.8)))
    block_factor = jnp.repeat(block_factor, TOK_DEV, axis=0)
    rate = jnp.where(delay_multiplier, 0.3 / LEAD_SPAN_LENGTH, 1.0 / 40.0)
    iteration_record = -rate[None, :] * per_step * block_factor
    spike_word_locations = jax.random.randint(spike_prng_seed, (3,), 0, LEAD_SPAN_LENGTH)
    objective_readings = jax.random.uniform(objective_prng_seed, (3, HEADS), jnp.float32, jnp.log(0.6), jnp.log(0.8))
    agreement_tally = (jnp.arange(LEAD_SPAN_LENGTH)[:, None] == spike_word_locations[None, :]).astype(jnp.float32)
    spike_addend = jnp.dot(agreement_tally, objective_readings)
    iteration_record = iteration_record + jnp.where(delay_multiplier[None, :], spike_addend, 0.0)
    return jnp.cumsum(iteration_record, axis=0)


def shard_levels(own_key, dims, shards, least, top_value):
    level = 1.0
    for dim, parts in shards:
        heights = jax.random.uniform(jax.random.fold_in(jax.random.fold_in(own_key, 6), dim), (parts,), jnp.float32, least / len(shards), top_value / len(shards))
        level = level * jnp.repeat(jnp.exp(heights), dims[dim] // parts).reshape((-1,) + (1,) * (len(dims) - 1 - dim))
    return level


def shared_out(stream_key, own, number, rows, number_of, top, most, slope):
    order = jax.random.permutation(stream_key, number_of)
    crowded, usual = load_shares(number_of, rows * top, most, slope, True), load_shares(number_of, rows * top, most, slope, False)
    places = jnp.arange(number_of)

    def named(sizes, offset_by):
        used = int((sizes > 0).sum())
        fixed = max(1, used // 4)
        moved = fixed + (places - fixed + offset_by * (used - fixed)) % max(1, number_of - fixed)
        return jnp.zeros((number_of,), jnp.int32).at[order[jnp.where(places < fixed, places, moved)]].set(jnp.asarray(sizes, jnp.int32))

    sizes = jnp.where(number % 4 == 0, named(crowded, number // 4), named(usual, number - number // 4 - 1))
    mixed = jax.random.permutation(jax.random.fold_in(own, 3), number_of)
    giver, taker = mixed[0:number_of // 2 * 2:2], mixed[1:number_of // 2 * 2:2]
    room = jnp.minimum(sizes[giver] - 1, most - sizes[taker]) // 2
    room = jnp.where((giver == order[0]) | (taker == order[0]) | (sizes[taker] == 0), 0, jnp.maximum(room, 0))
    moved = jax.random.randint(jax.random.fold_in(own, 4), (number_of // 2,), 0, 1 << 20) % (room + 1)
    sizes = sizes.at[giver].add(-moved).at[taker].add(moved)
    members = jnp.searchsorted(jnp.cumsum(sizes), jnp.arange(rows * top), side="right").astype(jnp.int32)
    grid = members.reshape(top, rows).T
    grid = grid[jax.random.permutation(jax.random.fold_in(own, 1), rows)]
    offset_by = jax.random.randint(jax.random.fold_in(own, 2), (rows, 1), 0, top)
    return jnp.take_along_axis(grid, (jnp.arange(top)[None, :] + offset_by) % top, axis=1)


def load_shares(amount, total, limit, slope, full):
    portions = [(1 << 20) // math.isqrt(grade ** slope) + 1 for grade in range(1, amount + 1)]
    largest = limit if full else min(limit, max(-(-total // amount), total * portions[0] // sum(portions)))
    least = 1 if total - largest >= amount - 1 else 0
    counts, spare = [largest] + [least] * (amount - 1), total - largest - least * (amount - 1)
    while spare > 0:
        candidates = [i for i in range(1, amount) if counts[i] < largest] or [i for i in range(1, amount) if counts[i] < limit]
        whole, remaining = sum([portions[i] for i in candidates]), spare
        for i in candidates:
            addition = min(limit - counts[i], max(1, remaining * portions[i] // whole), spare)
            counts[i] = counts[i] + addition
            spare = spare - addition
    return np.array(counts)


def centred(own_key, dims, scale, most, cuts=(), held_as=jnp.bfloat16):
    values = scale * jax.random.normal(own_key, dims, jnp.float32)
    if cuts:
        values = values * shard_levels(own_key, dims, cuts, -0.22, 0.18)
    return jnp.clip(values, -most, most).astype(held_as)


def setup_inputs(seed: int = 0) -> dict:
    seeds = jax.random.split(jax.random.key(seed), 13)
    queries = draw_queries(jax.random.fold_in(seeds[12], 71), 0)
    keys = draw_keys(jax.random.fold_in(seeds[12], 71), 0)
    values = centred(seeds[2], (LEAD_SPAN_LENGTH, KV * HD), 1.0, 6.0, ((0, 8), (1, 4)))
    log_gates = draw_log_gates(jax.random.fold_in(seeds[12], 71), 0)
    out_weight = centred(seeds[4], (HEADS * HD, D), (HEADS * HD) ** -0.5, 0.1875, ((0, 4),))
    moe_rows = centred(seeds[5], (MTOK, D), 1.0, 6.0, ((0, 8),))
    norm_gain = jnp.clip(1.0 + 0.18 * jax.random.normal(seeds[6], (D,), jnp.float32), 0.1, 1.9)
    experts_keys = jax.random.split(jax.random.fold_in(seeds[7], 1), MTOK // MOE_EP)
    experts_turns = jax.random.permutation(jax.random.fold_in(seeds[7], 3), MTOK // MOE_EP)
    experts = jax.vmap(lambda own, number: shared_out(jax.random.fold_in(seeds[7], 2), own, number, MOE_EP, EXPERTS, TOPK, CAP, 1))(experts_keys, experts_turns).reshape((MTOK, TOPK))
    expert_weights = jnp.clip(0.2 + 0.8 * jax.random.uniform(seeds[8], (MTOK, TOPK), jnp.float32) ** shard_levels(seeds[8], (MTOK, TOPK), ((0, 8),), -0.2, 0.2), 0.2, 1.0)
    w_gate = centred(seeds[9], (EXPERTS, D, FF), D ** -0.5, 0.125, ((0, 8), (2, 4)))
    w_up = centred(seeds[10], (EXPERTS, D, FF), D ** -0.5, 0.125, ((0, 8), (2, 4)))
    w_down = centred(seeds[11], (EXPERTS, FF, D), FF ** -0.5, 0.1875, ((0, 8), (1, 4)))
    return dict(queries=queries, keys=keys, values=values, log_gates=log_gates, out_weight=out_weight, moe_rows=moe_rows, norm_gain=norm_gain, experts=experts, expert_weights=expert_weights, w_gate=w_gate, w_up=w_up, w_down=w_down)


EPSILON = 1e-06

def split_sum(left, right, pieces):
    width = left.shape[1] // pieces
    total = jnp.zeros((left.shape[0], right.shape[1]), jnp.float32)
    for piece_index in range(pieces):
        partial_product = jnp.dot(left[:, piece_index * width:(piece_index + 1) * width], right[piece_index * width:(piece_index + 1) * width], preferred_element_type=jnp.float32)
        rounded = lax.optimization_barrier(partial_product.astype(jnp.bfloat16))
        total = total + rounded.astype(jnp.float32)
    return total.astype(jnp.bfloat16)

def reference(queries, keys, values, log_gates, out_weight, moe_rows, norm_gain, experts, expert_weights, w_gate, w_up, w_down):
    group = HEADS // KV
    query_heads = queries.reshape(LEAD_SPAN_LENGTH, KV, group, HD)
    key_heads = keys.reshape(LEAD_SPAN_LENGTH, KV, HD).astype(jnp.float32)
    value_heads = values.reshape(LEAD_SPAN_LENGTH, KV, HD).astype(jnp.float32)
    gate_lines = jnp.transpose(log_gates.reshape(LEAD_SPAN_LENGTH, KV, group), (1, 2, 0))
    query_span = math.gcd(LEAD_SPAN_LENGTH, 128)
    key_index = jnp.arange(LEAD_SPAN_LENGTH, dtype=jnp.int32)

    def attend(block_index):
        offset = block_index * query_span
        query_block = lax.dynamic_slice_in_dim(query_heads, offset, query_span, 0).astype(jnp.float32)
        query_gates = lax.dynamic_slice_in_dim(gate_lines, offset, query_span, 2)
        scores = jnp.einsum('qgrd,kgd->grqk', query_block, key_heads) * HD ** (-0.5)
        scores = scores + query_gates[..., None] - gate_lines[:, :, None, :]
        causal = key_index[None, :] <= (offset + jnp.arange(query_span, dtype=jnp.int32))[:, None]
        scores = jnp.where(causal, scores, -jnp.inf)
        highest = lax.optimization_barrier(jnp.max(scores, axis=-1, keepdims=True))
        weights = jnp.exp(scores - highest)
        totals = lax.optimization_barrier(jnp.sum(weights, axis=-1))
        rounded = lax.optimization_barrier(weights.astype(jnp.bfloat16)).astype(jnp.float32)
        heads_out = jnp.einsum('grqk,kgd->qgrd', rounded, value_heads)
        heads_out = heads_out / jnp.transpose(totals, (2, 0, 1))[..., None]
        return heads_out.reshape(query_span, HEADS * HD).astype(jnp.bfloat16)
    attended = lax.map(attend, jnp.arange(LEAD_SPAN_LENGTH // query_span, dtype=jnp.int32)).reshape(LEAD_SPAN_LENGTH, HEADS * HD)
    mixed = split_sum(attended, out_weight, N_TP)
    rows_float = moe_rows.astype(jnp.float32)
    normed = (rows_float * lax.rsqrt(lax.optimization_barrier(jnp.mean(rows_float * rows_float, axis=-1, keepdims=True)) + EPSILON) * norm_gain).astype(jnp.bfloat16)
    expert_ids = experts.reshape(N_EP, MOE_EP * TOPK)
    one_hot = (expert_ids[..., None] == jnp.arange(EXPERTS, dtype=jnp.int32)[None, None, :]).astype(jnp.int32)
    ranks = jnp.cumsum(one_hot, axis=1) - 1
    slot_index = lax.optimization_barrier(jnp.sum(one_hot * ranks, axis=-1)).astype(jnp.int32)
    source = jnp.arange(N_EP, dtype=jnp.int32)[:, None]
    destination = (expert_ids * (N_EP * CAP) + source * CAP + slot_index).reshape(-1).astype(jnp.int32)
    token_index = jnp.arange(MTOK * TOPK, dtype=jnp.int32) // TOPK
    buffer_rows = jnp.zeros((EXPERTS * N_EP * CAP, D), jnp.bfloat16).at[destination].set(normed[token_index])

    def run_expert(operands):
        rows, gate_weight, up_weight, down_weight = operands
        gate_part = jnp.dot(rows, gate_weight, preferred_element_type=jnp.float32)
        up_part = jnp.dot(rows, up_weight, preferred_element_type=jnp.float32)
        hidden = (jax.nn.silu(gate_part) * up_part).astype(jnp.bfloat16)
        return split_sum(hidden, down_weight, N_TP)
    results = lax.map(run_expert, (buffer_rows.reshape(EXPERTS, N_EP * CAP, D), w_gate, w_up, w_down))
    picked = results.reshape(EXPERTS * N_EP * CAP, D)[destination].reshape(MTOK, TOPK, D)
    moe_out = jnp.einsum('tk,tkd->td', expert_weights, picked.astype(jnp.float32)).astype(jnp.bfloat16)
    return (mixed, moe_out)
```

```python
import functools
import math

import jax
import jax.numpy as jnp
from jax import lax
from jax.experimental import pallas as pl
from jax.experimental.pallas import tpu as pltpu
from jax.sharding import PartitionSpec as P

D = 2048
HD = 64


EPSILON = 1e-06
MASKED = -1e30


def prepare_group(query_rows, gate_rows, positions, kv_here, group):
    rows = query_rows.shape[0]
    query_heads = query_rows.reshape(rows, kv_here, group, HD)
    query_gates = jnp.transpose(gate_rows.reshape(rows, kv_here, group), (1, 2, 0))
    return (query_heads, query_gates, positions)


def empty_state(rows, kv_here, group):
    return (
        jnp.full((kv_here, group, rows), MASKED, jnp.float32),
        jnp.zeros((kv_here, group, rows), jnp.float32),
        jnp.zeros((kv_here, group, rows, HD), jnp.float32),
    )


def attend_group(prepared, state, key_part, value_part, gate_part, offset, kv_here, group):
    query_heads, query_gates, query_position = prepared
    length = key_part.shape[0]
    key_span = math.gcd(length, 512)

    def run_blocks(start_state):

        def one_block(turn_index, inner):
            running_max, running_sum, weighted = inner
            first = turn_index * key_span
            key_block = lax.dynamic_slice_in_dim(key_part, first, key_span, 0).reshape(
                key_span, kv_here, HD
            )
            value_block = lax.dynamic_slice_in_dim(value_part, first, key_span, 0).reshape(
                key_span, kv_here, HD
            )
            gate_block = lax.dynamic_slice_in_dim(gate_part, first, key_span, 0).reshape(
                key_span, kv_here, group
            )
            scores = jnp.einsum(
                "qgrd,kgd->grqk", query_heads, key_block, preferred_element_type=jnp.float32
            ) * HD ** (-0.5)
            scores = (
                scores
                + query_gates[..., None]
                - jnp.transpose(gate_block, (1, 2, 0))[:, :, None, :]
            )
            key_position = first + jnp.arange(key_span, dtype=jnp.int32)
            scores = jnp.where(key_position[None, :] <= query_position[:, None], scores, MASKED)
            new_max = jnp.maximum(running_max, jnp.max(scores, axis=-1))
            weights = jnp.exp(scores - new_max[..., None])
            rescale = jnp.exp(running_max - new_max)
            running_sum = running_sum * rescale + jnp.sum(weights, axis=-1)
            weighted = weighted * rescale[..., None] + jnp.einsum(
                "grqk,kgd->grqd",
                weights.astype(jnp.bfloat16),
                value_block,
                preferred_element_type=jnp.float32,
            )
            return (new_max, running_sum, weighted)

        return lax.fori_loop(0, length // key_span, one_block, start_state)

    def keep_state(start_state):
        return start_state

    return lax.cond(offset <= query_position[-1], run_blocks, keep_state, state)


def finish_group(state, heads_here):
    running_max, running_sum, weighted = state
    rows = weighted.shape[2]
    attended = weighted / running_sum[..., None]
    return jnp.transpose(attended, (2, 0, 1, 3)).reshape(rows, heads_here * HD).astype(jnp.bfloat16)


def mixer_half(queries, keys, values, log_gates, out_weight):
    tok_rows = queries.shape[0]
    heads_here = log_gates.shape[1]
    kv_here = keys.shape[1] // HD
    group = heads_here // kv_here
    own_index = lax.axis_index("ep")
    positions = own_index * tok_rows + jnp.arange(tok_rows, dtype=jnp.int32)
    groups = [prepare_group(queries, log_gates, positions, kv_here, group)]
    initial = tuple((empty_state(entry[0].shape[0], kv_here, group) for entry in groups))
    offset = jnp.int32(0)
    key_part = lax.all_gather(keys.astype(jnp.float32), "ep", axis=0, tiled=True).astype(
        jnp.bfloat16
    )
    value_part = lax.all_gather(values.astype(jnp.float32), "ep", axis=0, tiled=True).astype(
        jnp.bfloat16
    )
    gate_part = lax.all_gather(log_gates, "ep", axis=0, tiled=True)
    states = tuple(
        (
            attend_group(
                groups[number],
                initial[number],
                key_part,
                value_part,
                gate_part,
                offset,
                kv_here,
                group,
            )
            for number in range(len(groups))
        )
    )
    finished = [finish_group(state, heads_here) for state in states]
    attended = finished[0]
    return lax.psum_scatter(
        jnp.dot(attended, out_weight, preferred_element_type=jnp.float32).astype(jnp.bfloat16),
        "tp",
        scatter_dimension=0,
        tiled=True,
    )


def experts_half(moe_rows, norm_gain, experts, expert_weights, w_gate, w_up, w_down):
    rows_here = moe_rows.shape[0]
    topk = experts.shape[1]
    experts_all = lax.axis_size("ep")
    capacity = 4 * rows_here // experts_all
    rows_float = moe_rows.astype(jnp.float32)
    normed = (
        rows_float
        * lax.rsqrt(jnp.mean(rows_float * rows_float, axis=-1, keepdims=True) + EPSILON)
        * norm_gain
    ).astype(jnp.bfloat16)
    expert_ids = experts.reshape(-1)
    one_hot = (expert_ids[:, None] == jnp.arange(experts_all, dtype=jnp.int32)[None, :]).astype(
        jnp.int32
    )
    ranks = jnp.cumsum(one_hot, axis=0) - 1
    slot_index = jnp.sum(one_hot * ranks, axis=1)
    destination = expert_ids * capacity + slot_index
    token_index = jnp.arange(rows_here * topk, dtype=jnp.int32) // topk
    width = D // lax.axis_size("tp")
    source_rows = lax.dynamic_slice_in_dim(normed, lax.axis_index("tp") * width, width, 1)
    outgoing = jnp.zeros((experts_all * capacity, source_rows.shape[1]), jnp.bfloat16)
    outgoing = (
        outgoing.at[destination]
        .set(source_rows[token_index])
        .reshape(experts_all, capacity, source_rows.shape[1])
    )
    arrived = lax.all_to_all(outgoing, "ep", split_axis=0, concat_axis=0, tiled=True)
    arrived = lax.all_gather(arrived, "tp", axis=2, tiled=True)
    slots = arrived.shape[1]
    flat_rows = arrived.reshape(-1, D)
    gate_part = jnp.dot(flat_rows, w_gate[0], preferred_element_type=jnp.float32)
    up_part = jnp.dot(flat_rows, w_up[0], preferred_element_type=jnp.float32)
    hidden = (jax.nn.silu(gate_part) * up_part).astype(jnp.bfloat16)
    partial_out = jnp.dot(hidden, w_down[0], preferred_element_type=jnp.float32).reshape(
        experts_all, slots, D
    )
    summed = lax.psum_scatter(
        partial_out.astype(jnp.bfloat16), "tp", scatter_dimension=2, tiled=True
    )
    returned = lax.all_to_all(summed, "ep", split_axis=0, concat_axis=0, tiled=True)
    picked = returned.reshape(experts_all * capacity, -1)[destination].reshape(rows_here, topk, -1)
    return jnp.einsum("tk,tkd->td", expert_weights, picked.astype(jnp.float32)).astype(jnp.bfloat16)


MESH = pl.DeviceIdType.MESH
VMEM_BUDGET = 56 * 2**20


def fits_fused(keys, log_gates, moe_rows, w_gate, experts):
    n_ep, n_tp = lax.axis_size("ep"), lax.axis_size("tp")
    rows_here, width = moe_rows.shape
    slots = n_ep * (4 * rows_here // n_ep)
    moved = 2 * (4 * slots * width + 3 * math.prod(w_gate.shape) + 8 * rows_here * width)
    return (
        n_tp == 4
        and n_ep == 8
        and w_gate.shape[0] == 1
        and experts.shape[1] == 2
        and 2 * keys.shape[1] == rows_here
        and 3 * log_gates.shape[1] <= 16
        and moved < VMEM_BUDGET
    )


def fused_kernel(
    n_ep,
    cap,
    kv_here,
    group,
    q_ref,
    blk_ref,
    qgate_ref,
    rows_ref,
    gain_ref,
    ext_ref,
    ex_ref,
    ew_ref,
    wo_hbm,
    wg_hbm,
    wu_hbm,
    wd_hbm,
    mixed_ref,
    moe_ref,
    wo,
    wg,
    wu,
    wd,
    nbuf,
    stage,
    buf,
    pbuf,
    in1,
    qown,
    qsend,
    in2,
    tot,
    ret,
    kv,
    att,
    mpart,
    min1,
    mq,
    min2,
    wsem,
    s_disp,
    r_disp,
    s_kv,
    r_kv,
    s_rs,
    r_rs,
    s_ret,
    r_ret,
    s_mix,
    r_mix,
):
    e = lax.axis_index("ep")
    j = lax.axis_index("tp")
    zs = n_ep // 2
    z, y = e // 2, e % 2
    mate = j + 1 - 2 * (j % 2)
    across = (j + 2) % 4
    diag = (mate + 2) % 4
    y_mate = 2 * z + 1 - y
    tok = rows_ref.shape[0]
    quarter = rows_ref.shape[1] // 4
    f32, bf16 = jnp.float32, jnp.bfloat16

    def remote(source, target, send, recv, to_ep, to_tp):
        return pltpu.make_async_remote_copy(
            src_ref=source,
            dst_ref=target,
            send_sem=send,
            recv_sem=recv,
            device_id=(to_ep, to_tp),
            device_id_type=MESH,
        )

    barrier = pltpu.get_barrier_semaphore()
    for d in range(1, n_ep):
        pl.semaphore_signal(barrier, inc=1, device_id=((e + d) % n_ep, j), device_id_type=MESH)
    for other in (mate, across):
        pl.semaphore_signal(barrier, inc=1, device_id=(e, other), device_id_type=MESH)
    weight_copies = [
        pltpu.make_async_copy(a, b, wsem.at[i])
        for i, (a, b) in enumerate(((wg_hbm, wg), (wu_hbm, wu), (wd_hbm, wd), (wo_hbm, wo)))
    ]
    for copy in weight_copies:
        copy.start()

    kv[e] = blk_ref[...]
    rows_float = rows_ref[...].astype(f32)
    scale = lax.rsqrt(jnp.mean(rows_float * rows_float, axis=-1, keepdims=True) + EPSILON)
    nbuf[...] = (rows_float * scale * gain_ref[...]).astype(bf16)

    row_i = lax.broadcasted_iota(jnp.int32, (tok, tok), 0)
    col_i = lax.broadcasted_iota(jnp.int32, (tok, tok), 1)
    upper = jnp.where(row_i < col_i, 1.0, 0.0).astype(bf16)
    lower = jnp.where(col_i < row_i, 1.0, 0.0).astype(bf16)
    names_t = lax.broadcasted_iota(jnp.int32, (n_ep, tok), 0)
    chosen_t = jnp.where(
        (names_t == ext_ref[0:1, :]) | (names_t == ext_ref[1:2, :]), 1.0, 0.0
    )
    rank_t = jnp.dot(chosen_t.astype(bf16), upper, preferred_element_type=f32)
    key_t = jnp.where(chosen_t > 0.5, rank_t, -1.0)
    slot_rows = lax.broadcasted_iota(jnp.int32, (cap, tok), 0).astype(f32)

    def pick(expert):
        line = jnp.sum(jnp.where(names_t == expert, key_t, 0.0), axis=0, keepdims=True)
        return jnp.where(slot_rows == line, 1.0, 0.0).astype(bf16)

    def slot(d):
        return pl.ds(d * cap, cap)

    pl.semaphore_wait(barrier, n_ep + 1)

    def kv_line(i):
        block = e - 2 * i
        return remote(
            kv.at[block], kv.at[block], s_kv.at[0, i], r_kv.at[0, i + 1], e + 2, j
        )

    def kv_side(i):
        block = e - 2 * i
        return remote(kv.at[block], kv.at[block], s_kv.at[1, i], r_kv.at[1, i], y_mate, j)

    def kv_line_arrival(i):
        block = e - 2 * i
        return remote(
            kv.at[block], kv.at[block], s_kv.at[0, i], r_kv.at[0, i], y_mate, j
        )

    def kv_step(i):
        if i == 0:

            @pl.when(z + 1 < zs)
            def _():
                kv_line(0).start()

            @pl.when(y == 0)
            def _():
                kv_side(0).start()

            return

        @pl.when(z >= i)
        def _():
            kv_line_arrival(i).wait_recv()

            @pl.when(z + 1 < zs)
            def _():
                kv_line(i).start()

            kv_side(i).start()

    def kv_finish():
        @pl.when(y == 1)
        def _():
            block = e - 1
            remote(
                kv.at[block], kv.at[block], s_kv.at[1, 0], r_kv.at[1, 0], y_mate, j
            ).wait_recv()

        for i in range(1, zs):

            @pl.when(z >= i)
            def _():
                block = 2 * (z - i) + 1 - y
                remote(
                    kv.at[block], kv.at[block], s_kv.at[1, i], r_kv.at[1, i], y_mate, j
                ).wait_recv()

    def kv_drain():
        for i in range(zs):

            @pl.when((z >= i) & (z + 1 < zs))
            def _():
                kv_line(i).wait_send()

            if i == 0:

                @pl.when(y == 0)
                def _():
                    kv_side(0).wait_send()
            else:

                @pl.when(z >= i)
                def _():
                    kv_side(i).wait_send()

    kv_step(0)

    own_columns = pl.ds(pl.multiple_of(j * quarter, quarter), quarter)
    first = {}
    for d in range(1, n_ep):
        to = (e + d) % n_ep
        stage[d - 1] = jnp.dot(
            pick(to), nbuf[:, own_columns], preferred_element_type=f32
        ).astype(bf16)
        first[d] = remote(
            stage.at[d - 1], buf.at[j, slot(d)], s_disp.at[0, d], r_disp.at[0, d], to, j
        )
        first[d].start()
    own_pick = pick(e)
    for part in range(4):
        buf[part, 0:cap, :] = jnp.dot(
            own_pick, nbuf[:, part * quarter : (part + 1) * quarter], preferred_element_type=f32
        ).astype(bf16)
    for copy in weight_copies:
        copy.wait()

    def spread(kind, part, d, to_tp):
        return remote(
            buf.at[part, slot(d)],
            buf.at[part, slot(d)],
            s_disp.at[kind, d],
            r_disp.at[kind, d],
            e,
            to_tp,
        )

    def arrive(d):
        first[d].wait_recv()
        spread(2, j, d, across).start()
        spread(1, j, d, mate).start()

    def relay(d):
        spread(2, across, d, across).wait_recv()
        spread(3, across, d, mate).start()

    def ready(d):
        if d:
            spread(1, mate, d, mate).wait_recv()
            spread(3, diag, d, mate).wait_recv()

    span = 2 * cap

    def rs_send(g):
        rows = pl.ds(g * span, span)
        return (
            remote(pbuf.at[mate, rows], in1.at[0, rows], s_rs.at[0, g], r_rs.at[0, g], e, mate),
            remote(pbuf.at[diag, rows], in1.at[1, rows], s_rs.at[1, g], r_rs.at[1, g], e, mate),
        )

    def rs_cross(g):
        rows = pl.ds(g * span, span)
        return remote(qsend.at[rows], in2.at[rows], s_rs.at[2, g], r_rs.at[2, g], e, across)

    def send_back(d):
        return remote(
            tot.at[slot(d)], ret.at[slot(d)], s_ret.at[d], r_ret.at[d], (e + n_ep - d) % n_ep, j
        )

    def compute(g):
        ready(2 * g)
        ready(2 * g + 1)
        rows = slice(g * span, (g + 1) * span)
        gate = jnp.zeros((span, wg.shape[1]), f32)
        up = jnp.zeros((span, wg.shape[1]), f32)
        for part in range(4):
            block = buf[part, rows, :]
            deep = slice(part * quarter, (part + 1) * quarter)
            gate = gate + jnp.dot(block, wg[deep, :], preferred_element_type=f32)
            up = up + jnp.dot(block, wu[deep, :], preferred_element_type=f32)
        hidden = (gate / (1.0 + jnp.exp(-gate)) * up).astype(bf16)
        for part in range(4):
            pbuf[part, rows, :] = jnp.dot(
                hidden, wd[:, part * quarter : (part + 1) * quarter], preferred_element_type=f32
            ).astype(bf16)
        for copy in reversed(rs_send(g)):
            copy.start()

    def fold(g):
        rows = slice(g * span, (g + 1) * span)
        one, two = rs_send(g)
        two.wait_recv()
        qsend[rows, :] = (
            pbuf[across, rows, :].astype(f32) + in1[1, rows, :].astype(f32)
        ).astype(bf16)
        rs_cross(g).start()
        one.wait_recv()

    def give(g):
        rows = slice(g * span, (g + 1) * span)
        rs_cross(g).wait_recv()
        total = (
            pbuf[j, rows, :].astype(f32)
            + in1[0, rows, :].astype(f32)
            + in2[rows, :].astype(f32)
        ).astype(bf16)
        tot[rows, :] = total
        for d in (2 * g, 2 * g + 1):
            if d:
                send_back(d).start()

    heads = kv_here * group
    hd = HD

    def attend(g):
        query = jnp.concatenate(
            [q_ref[:, (g * group + r) * hd : (g * group + r + 1) * hd] for r in range(group)], 0
        )
        qg = jnp.concatenate(
            [qgate_ref[:, g * group + r : g * group + r + 1] for r in range(group)], 0
        )
        qrow = jnp.concatenate(
            [lax.broadcasted_iota(jnp.int32, (tok, tok), 0) for r in range(group)], 0
        )
        kcol = lax.broadcasted_iota(jnp.int32, (group * tok, tok), 1)

        def one(b, state):
            top, total, acc = state
            k = kv[b, 0:tok, g * hd : (g + 1) * hd]
            v = kv[b, 0:tok, kv_here * hd + g * hd : kv_here * hd + (g + 1) * hd]
            gates = kv[b, tok : tok + 16, :].astype(f32)
            lines = gates[0:heads] + gates[heads : 2 * heads] + gates[2 * heads : 3 * heads]
            kg = jnp.concatenate(
                [
                    jnp.broadcast_to(lines[g * group + r : g * group + r + 1], (tok, tok))
                    for r in range(group)
                ],
                0,
            )
            scores = lax.dot_general(
                query, k, (((1,), (1,)), ((), ())), preferred_element_type=f32
            ) * (hd**-0.5)
            scores = scores + qg - kg
            scores = jnp.where(kcol + (b - e) * tok <= qrow, scores, MASKED)
            new_top = jnp.maximum(top, jnp.max(scores, axis=-1, keepdims=True))
            weights = jnp.exp(scores - new_top)
            rescale = jnp.exp(top - new_top)
            total = total * rescale + jnp.sum(weights, axis=-1, keepdims=True)
            acc = acc * rescale + jnp.dot(weights.astype(bf16), v, preferred_element_type=f32)
            return (new_top, total, acc)

        start = (
            jnp.full((group * tok, 1), MASKED, f32),
            jnp.zeros((group * tok, 1), f32),
            jnp.zeros((group * tok, hd), f32),
        )
        _, total, acc = lax.fori_loop(0, e + 1, one, start)
        out = (acc / total).astype(bf16)
        pieces = [out[r * tok : (r + 1) * tok] for r in range(group)]
        att[:, g * group * hd : (g + 1) * group * hd] = jnp.concatenate(pieces, 1)

    part_rows = tok // 4

    def mix_send():
        return (
            remote(mpart.at[mate], min1.at[0], s_mix.at[0], r_mix.at[0], e, mate),
            remote(mpart.at[diag], min1.at[1], s_mix.at[1], r_mix.at[1], e, mate),
        )

    def mix_cross():
        return remote(mq, min2, s_mix.at[2], r_mix.at[2], e, across)

    arrive(1)
    arrive(2)
    kv_step(1)
    relay(1)
    arrive(3)
    relay(2)
    compute(0)
    arrive(4)
    kv_step(2)
    relay(3)
    arrive(5)
    fold(0)
    relay(4)
    compute(1)
    arrive(6)
    kv_step(3)
    relay(5)
    arrive(7)
    fold(1)
    give(0)
    compute(2)
    relay(6)
    relay(7)
    fold(2)
    give(1)
    compute(3)
    kv_finish()
    fold(3)
    attend(0)
    give(2)
    attend(1)
    give(3)
    partial = jnp.dot(att[...], wo[...], preferred_element_type=f32).astype(bf16)
    for part in range(4):
        mpart[part] = partial[part * part_rows : (part + 1) * part_rows]
    for copy in reversed(mix_send()):
        copy.start()

    names = lax.broadcasted_iota(jnp.int32, (tok, n_ep), 1)
    chosen = jnp.where((names == ex_ref[:, 0:1]) | (names == ex_ref[:, 1:2]), 1.0, 0.0)
    rank = jnp.dot(lower, chosen.astype(bf16), preferred_element_type=f32)
    weight = jnp.where(names == ex_ref[:, 0:1], ew_ref[:, 0:1], 0.0) + jnp.where(
        names == ex_ref[:, 1:2], ew_ref[:, 1:2], 0.0
    )
    slot_columns = lax.broadcasted_iota(jnp.int32, (tok, cap), 1).astype(f32)

    one, two = mix_send()
    two.wait_recv()
    mq[...] = (mpart[across].astype(f32) + min1[1].astype(f32)).astype(bf16)
    mix_cross().start()
    one.wait_recv()

    combined = jnp.zeros((tok, quarter), f32)
    for d in range(n_ep):
        expert = (e + d) % n_ep
        mine = names == expert
        place = jnp.sum(jnp.where(mine, rank, 0.0), axis=1, keepdims=True)
        factor = jnp.sum(jnp.where(mine, weight, 0.0), axis=1, keepdims=True)
        spot = jnp.where(slot_columns == place, factor, 0.0)
        high = spot.astype(bf16)
        low = (spot - high.astype(f32)).astype(bf16)
        if d:
            send_back(d).wait_recv()
            came = ret[slot(d), :]
        else:
            came = tot[slot(0), :]
        combined = combined + jnp.dot(high, came, preferred_element_type=f32)
        combined = combined + jnp.dot(low, came, preferred_element_type=f32)
    moe_ref[...] = combined.astype(bf16)

    mix_cross().wait_recv()
    mixed_ref[...] = (
        mpart[j].astype(f32) + min1[0].astype(f32) + min2[...].astype(f32)
    ).astype(bf16)

    for d in range(1, n_ep):
        first[d].wait_send()
        spread(1, j, d, mate).wait_send()
        spread(2, j, d, across).wait_send()
        spread(3, across, d, mate).wait_send()
        send_back(d).wait_send()
    for g in range(n_ep // 2):
        for copy in (*rs_send(g), rs_cross(g)):
            copy.wait_send()
    for copy in (*mix_send(), mix_cross()):
        copy.wait_send()
    kv_drain()


def fused_layer(
    queries,
    keys,
    values,
    log_gates,
    out_weight,
    moe_rows,
    norm_gain,
    experts,
    expert_weights,
    w_gate,
    w_up,
    w_down,
):
    n_ep = lax.axis_size("ep")
    tok, width = moe_rows.shape
    quarter = width // 4
    cap = 4 * tok // n_ep
    slots = n_ep * cap
    kv_here = keys.shape[1] // HD
    group = log_gates.shape[1] // kv_here
    bf16, f32 = jnp.bfloat16, jnp.float32
    lines = log_gates.T
    high = lax.reduce_precision(lines, 8, 7)
    left = lines - high
    middle = lax.reduce_precision(left, 8, 7)
    gate_rows = jnp.concatenate([high, middle, left - middle], 0).astype(bf16)
    gate_rows = jnp.pad(gate_rows, ((0, 16 - gate_rows.shape[0]), (0, 0)))
    block = jnp.concatenate([jnp.concatenate([keys, values], 1), gate_rows], 0)
    dma, vmem = pltpu.SemaphoreType.DMA, pltpu.VMEM
    ff = w_gate.shape[2]
    heads_width = queries.shape[1]
    vm = pl.BlockSpec(memory_space=pltpu.VMEM)
    anywhere = pl.BlockSpec(memory_space=pl.ANY)
    return pl.pallas_call(
        functools.partial(fused_kernel, n_ep, cap, kv_here, group),
        out_shape=(
            jax.ShapeDtypeStruct((tok // 4, width), bf16),
            jax.ShapeDtypeStruct((tok, quarter), bf16),
        ),
        in_specs=[vm] * 8 + [anywhere] * 4,
        out_specs=(vm, vm),
        scratch_shapes=[
            vmem((heads_width, width), bf16),
            vmem((width, ff), bf16),
            vmem((width, ff), bf16),
            vmem((ff, width), bf16),
            vmem((tok, width), bf16),
            vmem((n_ep - 1, cap, quarter), bf16),
            vmem((4, slots, quarter), bf16),
            vmem((4, slots, quarter), bf16),
            vmem((2, slots, quarter), bf16),
            vmem((8, 128), bf16),
            vmem((slots, quarter), bf16),
            vmem((slots, quarter), bf16),
            vmem((slots, quarter), bf16),
            vmem((slots, quarter), bf16),
            vmem((n_ep, tok + 16, block.shape[1]), bf16),
            vmem((tok, heads_width), bf16),
            vmem((4, tok // 4, width), bf16),
            vmem((2, tok // 4, width), bf16),
            vmem((tok // 4, width), bf16),
            vmem((tok // 4, width), bf16),
            dma((4,)),
            dma((4, n_ep)),
            dma((4, n_ep)),
            dma((2, n_ep // 2 + 1)),
            dma((2, n_ep // 2 + 1)),
            dma((3, n_ep // 2)),
            dma((3, n_ep // 2)),
            dma((n_ep,)),
            dma((n_ep,)),
            dma((3,)),
            dma((3,)),
        ],
        compiler_params=pltpu.CompilerParams(
            collective_id=0, has_side_effects=True, vmem_limit_bytes=VMEM_BUDGET
        ),
    )(
        queries,
        block,
        log_gates,
        moe_rows,
        norm_gain.reshape(1, -1),
        experts.T,
        experts,
        expert_weights,
        out_weight,
        w_gate[0],
        w_up[0],
        w_down[0],
    )


def per_device(
    queries,
    keys,
    values,
    log_gates,
    out_weight,
    moe_rows,
    norm_gain,
    experts,
    expert_weights,
    w_gate,
    w_up,
    w_down,
):
    if fits_fused(keys, log_gates, moe_rows, w_gate, experts):
        return fused_layer(
            queries,
            keys,
            values,
            log_gates,
            out_weight,
            moe_rows,
            norm_gain,
            experts,
            expert_weights,
            w_gate,
            w_up,
            w_down,
        )
    mixed = mixer_half(queries, keys, values, log_gates, out_weight)
    moe_out = experts_half(moe_rows, norm_gain, experts, expert_weights, w_gate, w_up, w_down)
    return (mixed, moe_out)


def solution(mesh):
    placed = (
        P("ep", "tp"),
        P("ep", "tp"),
        P("ep", "tp"),
        P("ep", "tp"),
        P("tp", None),
        P("ep", None),
        P(),
        P("ep", None),
        P("ep", None),
        P("ep", None, "tp"),
        P("ep", None, "tp"),
        P("ep", "tp", None),
    )
    return jax.shard_map(
        per_device,
        mesh=mesh,
        in_specs=placed,
        out_specs=(P(("ep", "tp"), None), P("ep", "tp")),
        check_vma=False,
    )
```

```python
import functools
import math

import jax
import jax.numpy as jnp
from jax import lax
from jax.experimental import pallas as pl
from jax.experimental.pallas import tpu as pltpu
from jax.sharding import PartitionSpec as P

D = 2048
HD = 64


EPSILON = 1e-06
MASKED = -1e30


def prepare_group(query_rows, gate_rows, positions, kv_here, group):
    rows = query_rows.shape[0]
    query_heads = query_rows.reshape(rows, kv_here, group, HD)
    query_gates = jnp.transpose(gate_rows.reshape(rows, kv_here, group), (1, 2, 0))
    return (query_heads, query_gates, positions)


def empty_state(rows, kv_here, group):
    return (
        jnp.full((kv_here, group, rows), MASKED, jnp.float32),
        jnp.zeros((kv_here, group, rows), jnp.float32),
        jnp.zeros((kv_here, group, rows, HD), jnp.float32),
    )


def attend_group(prepared, state, key_part, value_part, gate_part, offset, kv_here, group):
    query_heads, query_gates, query_position = prepared
    length = key_part.shape[0]
    key_span = math.gcd(length, 512)

    def run_blocks(start_state):

        def one_block(turn_index, inner):
            running_max, running_sum, weighted = inner
            first = turn_index * key_span
            key_block = lax.dynamic_slice_in_dim(key_part, first, key_span, 0).reshape(
                key_span, kv_here, HD
            )
            value_block = lax.dynamic_slice_in_dim(value_part, first, key_span, 0).reshape(
                key_span, kv_here, HD
            )
            gate_block = lax.dynamic_slice_in_dim(gate_part, first, key_span, 0).reshape(
                key_span, kv_here, group
            )
            scores = jnp.einsum(
                "qgrd,kgd->grqk", query_heads, key_block, preferred_element_type=jnp.float32
            ) * HD ** (-0.5)
            scores = (
                scores
                + query_gates[..., None]
                - jnp.transpose(gate_block, (1, 2, 0))[:, :, None, :]
            )
            key_position = first + jnp.arange(key_span, dtype=jnp.int32)
            scores = jnp.where(key_position[None, :] <= query_position[:, None], scores, MASKED)
            new_max = jnp.maximum(running_max, jnp.max(scores, axis=-1))
            weights = jnp.exp(scores - new_max[..., None])
            rescale = jnp.exp(running_max - new_max)
            running_sum = running_sum * rescale + jnp.sum(weights, axis=-1)
            weighted = weighted * rescale[..., None] + jnp.einsum(
                "grqk,kgd->grqd",
                weights.astype(jnp.bfloat16),
                value_block,
                preferred_element_type=jnp.float32,
            )
            return (new_max, running_sum, weighted)

        return lax.fori_loop(0, length // key_span, one_block, start_state)

    def keep_state(start_state):
        return start_state

    return lax.cond(offset <= query_position[-1], run_blocks, keep_state, state)


def finish_group(state, heads_here):
    running_max, running_sum, weighted = state
    rows = weighted.shape[2]
    attended = weighted / running_sum[..., None]
    return jnp.transpose(attended, (2, 0, 1, 3)).reshape(rows, heads_here * HD).astype(jnp.bfloat16)


def mixer_half(queries, keys, values, log_gates, out_weight):
    tok_rows = queries.shape[0]
    heads_here = log_gates.shape[1]
    kv_here = keys.shape[1] // HD
    group = heads_here // kv_here
    own_index = lax.axis_index("ep")
    positions = own_index * tok_rows + jnp.arange(tok_rows, dtype=jnp.int32)
    groups = [prepare_group(queries, log_gates, positions, kv_here, group)]
    initial = tuple((empty_state(entry[0].shape[0], kv_here, group) for entry in groups))
    offset = jnp.int32(0)
    key_part = lax.all_gather(keys.astype(jnp.float32), "ep", axis=0, tiled=True).astype(
        jnp.bfloat16
    )
    value_part = lax.all_gather(values.astype(jnp.float32), "ep", axis=0, tiled=True).astype(
        jnp.bfloat16
    )
    gate_part = lax.all_gather(log_gates, "ep", axis=0, tiled=True)
    states = tuple(
        (
            attend_group(
                groups[number],
                initial[number],
                key_part,
                value_part,
                gate_part,
                offset,
                kv_here,
                group,
            )
            for number in range(len(groups))
        )
    )
    finished = [finish_group(state, heads_here) for state in states]
    attended = finished[0]
    return lax.psum_scatter(
        jnp.dot(attended, out_weight, preferred_element_type=jnp.float32).astype(jnp.bfloat16),
        "tp",
        scatter_dimension=0,
        tiled=True,
    )


def experts_half(moe_rows, norm_gain, experts, expert_weights, w_gate, w_up, w_down):
    rows_here = moe_rows.shape[0]
    topk = experts.shape[1]
    experts_all = lax.axis_size("ep")
    capacity = 4 * rows_here // experts_all
    rows_float = moe_rows.astype(jnp.float32)
    normed = (
        rows_float
        * lax.rsqrt(jnp.mean(rows_float * rows_float, axis=-1, keepdims=True) + EPSILON)
        * norm_gain
    ).astype(jnp.bfloat16)
    expert_ids = experts.reshape(-1)
    one_hot = (expert_ids[:, None] == jnp.arange(experts_all, dtype=jnp.int32)[None, :]).astype(
        jnp.int32
    )
    ranks = jnp.cumsum(one_hot, axis=0) - 1
    slot_index = jnp.sum(one_hot * ranks, axis=1)
    destination = expert_ids * capacity + slot_index
    token_index = jnp.arange(rows_here * topk, dtype=jnp.int32) // topk
    width = D // lax.axis_size("tp")
    source_rows = lax.dynamic_slice_in_dim(normed, lax.axis_index("tp") * width, width, 1)
    outgoing = jnp.zeros((experts_all * capacity, source_rows.shape[1]), jnp.bfloat16)
    outgoing = (
        outgoing.at[destination]
        .set(source_rows[token_index])
        .reshape(experts_all, capacity, source_rows.shape[1])
    )
    arrived = lax.all_to_all(outgoing, "ep", split_axis=0, concat_axis=0, tiled=True)
    arrived = lax.all_gather(arrived, "tp", axis=2, tiled=True)
    slots = arrived.shape[1]
    flat_rows = arrived.reshape(-1, D)
    gate_part = jnp.dot(flat_rows, w_gate[0], preferred_element_type=jnp.float32)
    up_part = jnp.dot(flat_rows, w_up[0], preferred_element_type=jnp.float32)
    hidden = (jax.nn.silu(gate_part) * up_part).astype(jnp.bfloat16)
    partial_out = jnp.dot(hidden, w_down[0], preferred_element_type=jnp.float32).reshape(
        experts_all, slots, D
    )
    summed = lax.psum_scatter(
        partial_out.astype(jnp.bfloat16), "tp", scatter_dimension=2, tiled=True
    )
    returned = lax.all_to_all(summed, "ep", split_axis=0, concat_axis=0, tiled=True)
    picked = returned.reshape(experts_all * capacity, -1)[destination].reshape(rows_here, topk, -1)
    return jnp.einsum("tk,tkd->td", expert_weights, picked.astype(jnp.float32)).astype(jnp.bfloat16)


MESH = pl.DeviceIdType.MESH
VMEM_BUDGET = 56 * 2**20


def fits_fused(keys, log_gates, moe_rows, w_gate, experts):
    n_ep, n_tp = lax.axis_size("ep"), lax.axis_size("tp")
    rows_here, width = moe_rows.shape
    slots = n_ep * (4 * rows_here // n_ep)
    moved = 2 * (4 * slots * width + 3 * math.prod(w_gate.shape) + 8 * rows_here * width)
    return (
        n_tp == 4
        and n_ep == 8
        and w_gate.shape[0] == 1
        and experts.shape[1] == 2
        and 2 * keys.shape[1] == rows_here
        and log_gates.shape[1] == 4
        and moved < VMEM_BUDGET
    )


def fused_kernel(
    n_ep,
    cap,
    kv_here,
    group,
    q_ref,
    k_ref,
    v_ref,
    small_ref,
    rows_ref,
    gain_ref,
    wo_hbm,
    wg_hbm,
    wu_hbm,
    wd_hbm,
    mixed_ref,
    moe_ref,
    wo,
    wg,
    wu,
    wd,
    nbuf,
    stage,
    buf,
    pbuf,
    in1,
    qown,
    qsend,
    in2,
    tot,
    ret,
    kv,
    tops,
    totals,
    accs,
    att,
    mpart,
    min1,
    mq,
    min2,
    wsem,
    s_disp,
    r_disp,
    s_kv,
    r_kv,
    s_rs,
    r_rs,
    s_ret,
    r_ret,
    s_mix,
    r_mix,
):
    e = lax.axis_index("ep")
    j = lax.axis_index("tp")
    zs = n_ep // 2
    z, y = e // 2, e % 2
    mate = j + 1 - 2 * (j % 2)
    across = (j + 2) % 4
    diag = (mate + 2) % 4
    y_mate = 2 * z + 1 - y
    tok = rows_ref.shape[0]
    quarter = rows_ref.shape[1] // 4
    f32, bf16 = jnp.float32, jnp.bfloat16

    def remote(source, target, send, recv, to_ep, to_tp):
        return pltpu.make_async_remote_copy(
            src_ref=source,
            dst_ref=target,
            send_sem=send,
            recv_sem=recv,
            device_id=(to_ep, to_tp),
            device_id_type=MESH,
        )

    barrier = pltpu.get_barrier_semaphore()
    for d in range(1, n_ep):
        pl.semaphore_signal(barrier, inc=1, device_id=((e + d) % n_ep, j), device_id_type=MESH)
    for other in (mate, across):
        pl.semaphore_signal(barrier, inc=1, device_id=(e, other), device_id_type=MESH)
    weight_copies = [
        pltpu.make_async_copy(a, b, wsem.at[i])
        for i, (a, b) in enumerate(((wg_hbm, wg), (wu_hbm, wu), (wd_hbm, wd), (wo_hbm, wo)))
    ]
    for copy in weight_copies:
        copy.start()

    heads = kv_here * group
    kv_width = k_ref.shape[1]
    kv[e, 0:tok, 0:kv_width] = k_ref[...]
    kv[e, 0:tok, kv_width : 2 * kv_width] = v_ref[...]
    small = small_ref[...]
    lines_high = small.astype(bf16).astype(f32)
    lines_left = small - lines_high
    lines_mid = lines_left.astype(bf16).astype(f32)
    kv[e, tok : tok + 32, :] = jnp.concatenate(
        [lines_high, lines_mid, lines_left - lines_mid, jnp.zeros_like(small)], 0
    ).astype(bf16)
    columns = jnp.transpose(small)
    ex_line = small.astype(jnp.int32)
    ex_column = columns.astype(jnp.int32)
    rows_float = rows_ref[...].astype(f32)
    scale = lax.rsqrt(jnp.mean(rows_float * rows_float, axis=-1, keepdims=True) + EPSILON)
    nbuf[...] = (rows_float * scale * gain_ref[...]).astype(bf16)

    row_i = lax.broadcasted_iota(jnp.int32, (tok, tok), 0)
    col_i = lax.broadcasted_iota(jnp.int32, (tok, tok), 1)
    upper = jnp.where(row_i < col_i, 1.0, 0.0).astype(bf16)
    lower = jnp.where(col_i < row_i, 1.0, 0.0).astype(bf16)
    names_t = lax.broadcasted_iota(jnp.int32, (n_ep, tok), 0)
    chosen_t = jnp.where(
        (names_t == ex_line[heads : heads + 1]) | (names_t == ex_line[heads + 1 : heads + 2]), 1.0, 0.0
    )
    rank_t = jnp.dot(chosen_t.astype(bf16), upper, preferred_element_type=f32)
    key_t = jnp.where(chosen_t > 0.5, rank_t, -1.0)
    slot_rows = lax.broadcasted_iota(jnp.int32, (cap, tok), 0).astype(f32)

    def pick(expert):
        line = jnp.sum(jnp.where(names_t == expert, key_t, 0.0), axis=0, keepdims=True)
        return jnp.where(slot_rows == line, 1.0, 0.0).astype(bf16)

    def slot(d):
        return pl.ds(d * cap, cap)

    pl.semaphore_wait(barrier, n_ep + 1)

    def kv_line(i):
        block = e - 2 * i
        return remote(
            kv.at[block], kv.at[block], s_kv.at[0, i], r_kv.at[0, i + 1], e + 2, j
        )

    def kv_side(i):
        block = e - 2 * i
        return remote(kv.at[block], kv.at[block], s_kv.at[1, i], r_kv.at[1, i], y_mate, j)

    def kv_line_arrival(i):
        block = e - 2 * i
        return remote(
            kv.at[block], kv.at[block], s_kv.at[0, i], r_kv.at[0, i], y_mate, j
        )

    def kv_step(i):
        if i == 0:

            @pl.when(z + 1 < zs)
            def _():
                kv_line(0).start()

            @pl.when(y == 0)
            def _():
                kv_side(0).start()

            return

        @pl.when(z >= i)
        def _():
            kv_line_arrival(i).wait_recv()

            @pl.when(z + 1 < zs)
            def _():
                kv_line(i).start()

            kv_side(i).start()

    def side_wait(i):
        @pl.when((y == 1) if i == 0 else (z >= i))
        def _():
            block = 2 * (z - i) + 1 - y
            remote(
                kv.at[block], kv.at[block], s_kv.at[1, i], r_kv.at[1, i], y_mate, j
            ).wait_recv()

    def kv_drain():
        for i in range(zs):

            @pl.when((z >= i) & (z + 1 < zs))
            def _():
                kv_line(i).wait_send()

            if i == 0:

                @pl.when(y == 0)
                def _():
                    kv_side(0).wait_send()
            else:

                @pl.when(z >= i)
                def _():
                    kv_side(i).wait_send()

    kv_step(0)

    own_columns = pl.ds(pl.multiple_of(j * quarter, quarter), quarter)
    first = {}
    for d in range(1, n_ep):
        to = (e + d) % n_ep
        stage[d - 1] = jnp.dot(
            pick(to), nbuf[:, own_columns], preferred_element_type=f32
        ).astype(bf16)
        first[d] = remote(
            stage.at[d - 1], buf.at[j, slot(d)], s_disp.at[0, d], r_disp.at[0, d], to, j
        )
        first[d].start()
    own_pick = pick(e)
    for part in range(4):
        buf[part, 0:cap, :] = jnp.dot(
            own_pick, nbuf[:, part * quarter : (part + 1) * quarter], preferred_element_type=f32
        ).astype(bf16)

    def spread(kind, part, d, to_tp):
        return remote(
            buf.at[part, slot(d)],
            buf.at[part, slot(d)],
            s_disp.at[kind, d],
            r_disp.at[kind, d],
            e,
            to_tp,
        )

    def arrive(d):
        first[d].wait_recv()
        spread(2, j, d, across).start()
        spread(1, j, d, mate).start()

    def relay(d):
        spread(2, across, d, across).wait_recv()
        spread(3, across, d, mate).start()

    def ready(d):
        if d:
            spread(1, mate, d, mate).wait_recv()
            spread(3, diag, d, mate).wait_recv()

    span = 2 * cap

    def rs_send(g):
        rows = pl.ds(g * span, span)
        return (
            remote(pbuf.at[mate, rows], in1.at[0, rows], s_rs.at[0, g], r_rs.at[0, g], e, mate),
            remote(pbuf.at[diag, rows], in1.at[1, rows], s_rs.at[1, g], r_rs.at[1, g], e, mate),
        )

    def rs_cross(g):
        rows = pl.ds(g * span, span)
        return remote(qsend.at[rows], in2.at[rows], s_rs.at[2, g], r_rs.at[2, g], e, across)

    def send_back(d):
        return remote(
            tot.at[slot(d)], ret.at[slot(d)], s_ret.at[d], r_ret.at[d], (e + n_ep - d) % n_ep, j
        )

    def compute(g):
        ready(2 * g)
        ready(2 * g + 1)
        rows = slice(g * span, (g + 1) * span)
        gate = jnp.zeros((span, wg.shape[1]), f32)
        up = jnp.zeros((span, wg.shape[1]), f32)
        for part in range(4):
            block = buf[part, rows, :]
            deep = slice(part * quarter, (part + 1) * quarter)
            gate = gate + jnp.dot(block, wg[deep, :], preferred_element_type=f32)
            up = up + jnp.dot(block, wu[deep, :], preferred_element_type=f32)
        hidden = (gate / (1.0 + jnp.exp(-gate)) * up).astype(bf16)
        for part in range(4):
            pbuf[part, rows, :] = jnp.dot(
                hidden, wd[:, part * quarter : (part + 1) * quarter], preferred_element_type=f32
            ).astype(bf16)
        for copy in reversed(rs_send(g)):
            copy.start()

    def fold(g):
        rows = slice(g * span, (g + 1) * span)
        one, two = rs_send(g)
        two.wait_recv()
        qsend[rows, :] = (
            pbuf[across, rows, :].astype(f32) + in1[1, rows, :].astype(f32)
        ).astype(bf16)
        rs_cross(g).start()
        one.wait_recv()

    def give(g):
        rows = slice(g * span, (g + 1) * span)
        rs_cross(g).wait_recv()
        total = (
            pbuf[j, rows, :].astype(f32)
            + in1[0, rows, :].astype(f32)
            + in2[rows, :].astype(f32)
        ).astype(bf16)
        tot[rows, :] = total
        for d in (2 * g, 2 * g + 1):
            if d:
                send_back(d).start()

    hd = HD

    def attend(block, own):
        gates = kv[block, tok : tok + 32, :].astype(f32)
        lines = gates[0:8] + gates[8:16] + gates[16:24]
        for h in range(heads):
            g = h // group
            query = (q_ref[:, h * hd : (h + 1) * hd].astype(f32) * hd**-0.5).astype(bf16)
            k = kv[block, 0:tok, g * hd : (g + 1) * hd]
            v = kv[block, 0:tok, kv_width + g * hd : kv_width + (g + 1) * hd]
            scores = lax.dot_general(
                query, k, (((1,), (1,)), ((), ())), preferred_element_type=f32
            )
            scores = scores + columns[:, h : h + 1] - lines[h : h + 1]
            if own:
                scores = jnp.where(col_i <= row_i, scores, MASKED)
            new_top = jnp.max(scores, axis=-1, keepdims=True)
            if not own:
                new_top = jnp.maximum(tops[h], new_top)
            weights = jnp.exp(scores - new_top)
            total = jnp.sum(weights, axis=-1, keepdims=True)
            acc = jnp.dot(weights.astype(bf16), v, preferred_element_type=f32)
            if not own:
                rescale = jnp.exp(tops[h] - new_top)
                total = total + totals[h] * rescale
                acc = acc + accs[h] * rescale
            tops[h] = new_top
            totals[h] = total
            accs[h] = acc

    def stage_attention(i):
        if i == 1:
            side_wait(0)
            low, high = 2 * jnp.maximum(z - 1, 0), e
        else:
            low = 2 * jnp.maximum(z - i, 0)
            high = 2 * jnp.maximum(z - i + 1, 0)
        side_wait(i)

        def one(block, carry):
            attend(block, False)
            return carry

        lax.fori_loop(low, high, one, 0)

    part_rows = tok // 4

    def mix_send():
        return (
            remote(mpart.at[mate], min1.at[0], s_mix.at[0], r_mix.at[0], e, mate),
            remote(mpart.at[diag], min1.at[1], s_mix.at[1], r_mix.at[1], e, mate),
        )

    def mix_cross():
        return remote(mq, min2, s_mix.at[2], r_mix.at[2], e, across)

    attend(e, True)
    arrive(1)
    arrive(2)
    kv_step(1)
    relay(1)
    arrive(3)
    relay(2)
    for copy in weight_copies:
        copy.wait()
    compute(0)
    arrive(4)
    kv_step(2)
    relay(3)
    arrive(5)
    fold(0)
    relay(4)
    compute(1)
    arrive(6)
    kv_step(3)
    relay(5)
    give(0)
    stage_attention(1)
    arrive(7)
    relay(6)
    fold(1)
    relay(7)
    compute(2)
    give(1)
    compute(3)
    fold(2)
    stage_attention(2)
    give(2)
    fold(3)
    stage_attention(3)
    for h in range(0, heads, 2):
        att[:, h * hd : (h + 2) * hd] = jnp.concatenate(
            [accs[h] / totals[h], accs[h + 1] / totals[h + 1]], 1
        ).astype(bf16)
    partial = jnp.dot(att[...], wo[...], preferred_element_type=f32).astype(bf16)
    for part in range(4):
        mpart[part] = partial[part * part_rows : (part + 1) * part_rows]
    for copy in reversed(mix_send()):
        copy.start()

    give(3)
    names = lax.broadcasted_iota(jnp.int32, (tok, n_ep), 1)
    first_name, second_name = (ex_column[:, heads + k : heads + k + 1] for k in range(2))
    first_weight, second_weight = (columns[:, heads + k : heads + k + 1] for k in (2, 3))
    chosen = jnp.where((names == first_name) | (names == second_name), 1.0, 0.0)
    rank = jnp.dot(lower, chosen.astype(bf16), preferred_element_type=f32)
    weight = jnp.where(names == first_name, first_weight, 0.0) + jnp.where(
        names == second_name, second_weight, 0.0
    )
    slot_columns = lax.broadcasted_iota(jnp.int32, (tok, cap), 1).astype(f32)

    one, two = mix_send()
    two.wait_recv()
    mq[...] = (mpart[across].astype(f32) + min1[1].astype(f32)).astype(bf16)
    mix_cross().start()
    one.wait_recv()

    combined = jnp.zeros((tok, quarter), f32)
    for d in range(n_ep):
        expert = (e + d) % n_ep
        mine = names == expert
        place = jnp.sum(jnp.where(mine, rank, 0.0), axis=1, keepdims=True)
        factor = jnp.sum(jnp.where(mine, weight, 0.0), axis=1, keepdims=True)
        spot = jnp.where(slot_columns == place, factor, 0.0)
        high = spot.astype(bf16)
        low = (spot - high.astype(f32)).astype(bf16)
        if d:
            send_back(d).wait_recv()
            came = ret[slot(d), :]
        else:
            came = tot[slot(0), :]
        combined = combined + jnp.dot(high, came, preferred_element_type=f32)
        combined = combined + jnp.dot(low, came, preferred_element_type=f32)
    moe_ref[...] = combined.astype(bf16)

    mix_cross().wait_recv()
    mixed_ref[...] = (
        mpart[j].astype(f32) + min1[0].astype(f32) + min2[...].astype(f32)
    ).astype(bf16)

    for d in range(1, n_ep):
        first[d].wait_send()
        spread(1, j, d, mate).wait_send()
        spread(2, j, d, across).wait_send()
        spread(3, across, d, mate).wait_send()
        send_back(d).wait_send()
    for g in range(n_ep // 2):
        for copy in (*rs_send(g), rs_cross(g)):
            copy.wait_send()
    for copy in (*mix_send(), mix_cross()):
        copy.wait_send()
    kv_drain()


def fused_layer(
    queries,
    keys,
    values,
    log_gates,
    out_weight,
    moe_rows,
    norm_gain,
    experts,
    expert_weights,
    w_gate,
    w_up,
    w_down,
):
    n_ep = lax.axis_size("ep")
    tok, width = moe_rows.shape
    quarter = width // 4
    cap = 4 * tok // n_ep
    slots = n_ep * cap
    kv_here = keys.shape[1] // HD
    group = log_gates.shape[1] // kv_here
    bf16, f32 = jnp.bfloat16, jnp.float32
    small = jnp.concatenate([log_gates, experts.astype(f32), expert_weights], 1).T
    dma, vmem = pltpu.SemaphoreType.DMA, pltpu.VMEM
    ff = w_gate.shape[2]
    heads_width = queries.shape[1]
    vm = pl.BlockSpec(memory_space=pltpu.VMEM)
    anywhere = pl.BlockSpec(memory_space=pl.ANY)
    return pl.pallas_call(
        functools.partial(fused_kernel, n_ep, cap, kv_here, group),
        out_shape=(
            jax.ShapeDtypeStruct((tok // 4, width), bf16),
            jax.ShapeDtypeStruct((tok, quarter), bf16),
        ),
        in_specs=[vm] * 6 + [anywhere] * 4,
        out_specs=(vm, vm),
        scratch_shapes=[
            vmem((heads_width, width), bf16),
            vmem((width, ff), bf16),
            vmem((width, ff), bf16),
            vmem((ff, width), bf16),
            vmem((tok, width), bf16),
            vmem((n_ep - 1, cap, quarter), bf16),
            vmem((4, slots, quarter), bf16),
            vmem((4, slots, quarter), bf16),
            vmem((2, slots, quarter), bf16),
            vmem((8, 128), bf16),
            vmem((slots, quarter), bf16),
            vmem((slots, quarter), bf16),
            vmem((slots, quarter), bf16),
            vmem((slots, quarter), bf16),
            vmem((n_ep, tok + 32, tok), bf16),
            vmem((kv_here * group, tok, 1), f32),
            vmem((kv_here * group, tok, 1), f32),
            vmem((kv_here * group, tok, HD), f32),
            vmem((tok, heads_width), bf16),
            vmem((4, tok // 4, width), bf16),
            vmem((2, tok // 4, width), bf16),
            vmem((tok // 4, width), bf16),
            vmem((tok // 4, width), bf16),
            dma((4,)),
            dma((4, n_ep)),
            dma((4, n_ep)),
            dma((2, n_ep // 2 + 1)),
            dma((2, n_ep // 2 + 1)),
            dma((3, n_ep // 2)),
            dma((3, n_ep // 2)),
            dma((n_ep,)),
            dma((n_ep,)),
            dma((3,)),
            dma((3,)),
        ],
        compiler_params=pltpu.CompilerParams(
            collective_id=0, has_side_effects=True, vmem_limit_bytes=VMEM_BUDGET
        ),
    )(
        queries,
        keys,
        values,
        small,
        moe_rows,
        norm_gain.reshape(1, -1),
        out_weight,
        w_gate[0],
        w_up[0],
        w_down[0],
    )


def per_device(
    queries,
    keys,
    values,
    log_gates,
    out_weight,
    moe_rows,
    norm_gain,
    experts,
    expert_weights,
    w_gate,
    w_up,
    w_down,
):
    if fits_fused(keys, log_gates, moe_rows, w_gate, experts):
        return fused_layer(
            queries,
            keys,
            values,
            log_gates,
            out_weight,
            moe_rows,
            norm_gain,
            experts,
            expert_weights,
            w_gate,
            w_up,
            w_down,
        )
    mixed = mixer_half(queries, keys, values, log_gates, out_weight)
    moe_out = experts_half(moe_rows, norm_gain, experts, expert_weights, w_gate, w_up, w_down)
    return (mixed, moe_out)


def solution(mesh):
    placed = (
        P("ep", "tp"),
        P("ep", "tp"),
        P("ep", "tp"),
        P("ep", "tp"),
        P("tp", None),
        P("ep", None),
        P(),
        P("ep", None),
        P("ep", None),
        P("ep", None, "tp"),
        P("ep", None, "tp"),
        P("ep", "tp", None),
    )
    return jax.shard_map(
        per_device,
        mesh=mesh,
        in_specs=placed,
        out_specs=(P(("ep", "tp"), None), P("ep", "tp")),
        check_vma=False,
    )
```
